32 devices in a mesh: sp: 8 (over z, x), tp: 4 (over y, core).
Axes of the slice: x: 2, y: 2, z: 4, core: 2. Of those that a mesh axis runs over, the one named last changes fastest.
Arguments:
- queries: bfloat16 [1024, 2048], P('sp', 'tp'), may hold values from -440 to 440
- key_rows: bfloat16 [1024, 1024], P('sp', 'tp'), may hold values from -6 to 6
- value_rows: bfloat16 [1024, 1024], P('sp', 'tp'), may hold values from -6 to 6
- sink_logits: float32 [32], P('tp'), may hold values from -6 to 6
- out_weight: bfloat16 [2048, 2048], P('tp'), may hold values from -0.125 to 0.125
- residual: bfloat16 [1024, 2048], P('sp'), may hold values from -3 to 3
- norm_gain: float32 [2048], replicated, may hold values from 0.1 to 1.9
- routes: int32 [1024, 2], P('sp'), may hold values from 0 to 7, all different within a row; in each aligned block of 128 rows (0 to 127, 128 to 255, ...) at most 64 rows name the same one
- route_weights: float32 [1024, 2], P('sp'), may hold values from 0.2 to 1
- gate_weight: bfloat16 [8, 2048, 4096], P('sp', None, 'tp'), may hold values from -0.125 to 0.125
- up_weight: bfloat16 [8, 2048, 4096], P('sp', None, 'tp'), may hold values from -0.125 to 0.125
- down_weight: bfloat16 [8, 4096, 2048], P('sp', 'tp'), may hold values from -0.09375 to 0.09375
Outputs:
- layer_out: bfloat16 [1024, 2048], P('sp')
The draws below stay inside these ranges and needn't reach their ends.
Inputs may be any that keep to these rules, and one draw needn't show every extreme that they name: `routes`: each row names 2 different experts. In each aligned block of 128 rows (the rows of one index of sp) no expert is named by more than 64 rows, a bound that some block reaches.
All inputs are finite; a program needn't handle non-finite values.
Results may differ from the reference program's by a relative error of at most 0.02.
Values may be sent and summed in bfloat16 or wider, within the bound.
A program may use at most 64 MiB of HBM per device.

```python
import math
import jax
import jax.numpy as jnp
import numpy as np
from jax import lax

D = 2048
HEAD_DIM = 64
QH = 32
KVH = 16
WINDOW = 128
FF = 4096
TOP = 2
TOK_DEV = 128
TOKENS = 1024
EXPERTS = 8
CAP = 64
N_SP = 8
N_TP = 4


def plant_keys(key):
    key_draw = jax.random.normal(jax.random.fold_in(key, 7), (TOKENS, KVH * HEAD_DIM), jnp.float32)
    return jnp.clip(key_draw, -6.0, 6.0)


def draw_key_rows(key, part):
    key_draw = plant_keys(key)
    return key_draw.astype(jnp.bfloat16)


def draw_queries(key, part):
    base = jax.random.normal(jax.random.fold_in(key, 8), (TOKENS, QH * HEAD_DIM), jnp.float32)
    base = jnp.clip(base, -6.0, 6.0)
    return base.astype(jnp.bfloat16)


def levels(key, extent, cuts, smallest, top_value):
    level = 1.0
    for axis_at, shards_of in cuts:
        steps = jax.random.uniform(jax.random.fold_in(jax.random.fold_in(key, 6), axis_at), (shards_of,), jnp.float32, smallest / len(cuts), top_value / len(cuts))
        level = level * jnp.repeat(jnp.exp(steps), extent[axis_at] // shards_of).reshape((-1,) + (1,) * (len(extent) - 1 - axis_at))
    return level


def deal_out(rng, own, number, rows, amount, top, limit, skew):
    ranking = jax.random.permutation(rng, amount)
    heavy_load, common = portions_of(amount, rows * top, limit, skew, True), portions_of(amount, rows * top, limit, skew, False)
    places = jnp.arange(amount)

    def named(tallies, turn):
        used = int((tallies > 0).sum())
        fixed = max(1, used // 4)
        moved = fixed + (places - fixed + turn * (used - fixed)) % max(1, amount - fixed)
        return jnp.zeros((amount,), jnp.int32).at[ranking[jnp.where(places < fixed, places, moved)]].set(jnp.asarray(tallies, jnp.int32))

    tallies = jnp.where(number % 4 == 0, named(heavy_load, number // 4), named(common, number - number // 4 - 1))
    mixed = jax.random.permutation(jax.random.fold_in(own, 3), amount)
    source_of, taker = mixed[0:amount // 2 * 2:2], mixed[1:amount // 2 * 2:2]
    margin = jnp.minimum(tallies[source_of] - 1, limit - tallies[taker]) // 2
    margin = jnp.where((source_of == ranking[0]) | (taker == ranking[0]) | (tallies[taker] == 0), 0, jnp.maximum(margin, 0))
    moved = jax.random.randint(jax.random.fold_in(own, 4), (amount // 2,), 0, 1 << 20) % (margin + 1)
    tallies = tallies.at[source_of].add(-moved).at[taker].add(moved)
    items = jnp.searchsorted(jnp.cumsum(tallies), jnp.arange(rows * top), side="right").astype(jnp.int32)
    grid = items.reshape(top, rows).T
    grid = grid[jax.random.permutation(jax.random.fold_in(own, 1), rows)]
    turn = jax.random.randint(jax.random.fold_in(own, 2), (rows, 1), 0, top)
    return jnp.take_along_axis(grid, (jnp.arange(top)[None, :] + turn) % top, axis=1)


def portions_of(amount, total, limit, slope, full):
    weights = [(1 << 20) // math.isqrt(standing ** slope) + 1 for standing in range(1, amount + 1)]
    largest = limit if full else min(limit, max(-(-total // amount), total * weights[0] // sum(weights)))
    least = 1 if total - largest >= amount - 1 else 0
    counts, surplus = [largest] + [least] * (amount - 1), total - largest - least * (amount - 1)
    while surplus > 0:
        movable = [i for i in range(1, amount) if counts[i] < largest] or [i for i in range(1, amount) if counts[i] < limit]
        whole, left = sum([weights[i] for i in movable]), surplus
        for i in movable:
            addition = min(limit - counts[i], max(1, left * weights[i] // whole), surplus)
            counts[i] = counts[i] + addition
            surplus = surplus - addition
    return np.array(counts)


def noise(rng, extent, deviation, limit, shards=(), kind=jnp.bfloat16):
    level = levels(rng, extent, shards, -0.22, 0.18) if shards else 1.0
    result = jax.random.normal(rng, extent, jnp.float32) * deviation * level
    return jnp.minimum(jnp.maximum(result, -limit), limit).astype(kind)


def setup_inputs(seed: int = 0) -> dict:
    key_of = jax.random.split(jax.random.key(seed), 13)
    queries = draw_queries(jax.random.fold_in(key_of[12], 71), 0)
    key_rows = draw_key_rows(jax.random.fold_in(key_of[12], 71), 0)
    value_rows = noise(key_of[2], (TOKENS, KVH * HEAD_DIM), 1.0, 6.0, ((0, 8), (1, 4)))
    sink_logits = noise(key_of[3], (QH,), 2.0, 6.0, ((0, 4),), jnp.float32)
    out_weight = noise(key_of[4], (QH * HEAD_DIM, D), (QH * HEAD_DIM) ** -0.5, 0.125, ((0, 4),))
    residual = noise(key_of[5], (TOKENS, D), 0.5, 3.0, ((0, 8),))
    norm_gain = jnp.clip(1.0 + 0.18 * jax.random.normal(key_of[6], (D,), jnp.float32), 0.1, 1.9)
    routes_keys = jax.random.split(jax.random.fold_in(key_of[7], 1), TOKENS // TOK_DEV)
    routes_turns = jax.random.permutation(jax.random.fold_in(key_of[7], 3), TOKENS // TOK_DEV)
    routes = jax.vmap(lambda own, number: deal_out(jax.random.fold_in(key_of[7], 2), own, number, TOK_DEV, EXPERTS, TOP, CAP, 1))(routes_keys, routes_turns).reshape((TOKENS, TOP))
    route_weights = jnp.clip(0.2 + 0.8 * jax.random.uniform(key_of[8], (TOKENS, TOP), jnp.float32) ** levels(key_of[8], (TOKENS, TOP), ((0, 8),), -0.2, 0.2), 0.2, 1.0)
    gate_weight = noise(key_of[9], (EXPERTS, D, FF), D ** -0.5, 0.125, ((0, 8), (2, 4)))
    up_weight = noise(key_of[10], (EXPERTS, D, FF), D ** -0.5, 0.125, ((0, 8), (2, 4)))
    down_weight = noise(key_of[11], (EXPERTS, FF, D), FF ** -0.5, 0.09375, ((0, 8), (1, 4)))
    return dict(queries=queries, key_rows=key_rows, value_rows=value_rows, sink_logits=sink_logits, out_weight=out_weight, residual=residual, norm_gain=norm_gain, routes=routes, route_weights=route_weights, gate_weight=gate_weight, up_weight=up_weight, down_weight=down_weight)


def reference(queries, key_rows, value_rows, sink_logits, out_weight, residual, norm_gain, routes, route_weights, gate_weight, up_weight, down_weight):
    blocks = TOKENS // WINDOW
    group_size = QH // KVH
    zeros_rim = jnp.zeros((WINDOW, KVH * HEAD_DIM), jnp.bfloat16)
    key_ext = jnp.concatenate([zeros_rim, key_rows], axis=0).reshape(blocks + 1, WINDOW, KVH, HEAD_DIM)
    val_ext = jnp.concatenate([zeros_rim, value_rows], axis=0).reshape(blocks + 1, WINDOW, KVH, HEAD_DIM)
    key_pair = jnp.concatenate([key_ext[:-1], key_ext[1:]], axis=1)
    val_pair = jnp.concatenate([val_ext[:-1], val_ext[1:]], axis=1)
    query_blocks = queries.reshape(blocks, WINDOW, KVH, group_size, HEAD_DIM)
    distance = jnp.arange(WINDOW)[:, None] + WINDOW - jnp.arange(2 * WINDOW)[None, :]
    key_global = jnp.arange(blocks)[:, None, None] * WINDOW + jnp.arange(2 * WINDOW)[None, None, :] - WINDOW
    allowed = (distance >= 0)[None] & (distance <= WINDOW)[None] & (key_global >= 0)
    head_ids = jnp.arange(QH)
    slopes = jnp.exp2(-8.0 * (head_ids + 1).astype(jnp.float32) / QH).reshape(KVH, group_size)

    def attend_head(inputs):
        q_head, k_head, v_head, sink_head, slope_head = inputs
        scores = jnp.einsum('bqgd,bcd->bgqc', q_head.astype(jnp.float32), k_head.astype(jnp.float32)) * HEAD_DIM ** (-0.5)
        scores = scores - slope_head[None, :, None, None] * distance.astype(jnp.float32)
        scores = jnp.where(allowed[:, None], scores, -jnp.inf)
        row_peak = lax.optimization_barrier(jnp.max(scores, axis=-1, keepdims=True))
        log_total = row_peak + jnp.log(lax.optimization_barrier(jnp.sum(jnp.exp(scores - row_peak), axis=-1, keepdims=True)))
        probs = jnp.exp(scores - log_total).astype(jnp.bfloat16)
        mixed = jnp.einsum('bgqc,bcd->bqgd', probs.astype(jnp.float32), v_head.astype(jnp.float32))
        keep_factor = jax.nn.sigmoid(log_total[..., 0] - sink_head[None, :, None])
        keep_factor = jnp.transpose(keep_factor, (0, 2, 1))[..., None]
        return (mixed * keep_factor).astype(jnp.bfloat16)
    per_head = lax.map(attend_head, (jnp.moveaxis(query_blocks, 2, 0), jnp.moveaxis(key_pair, 2, 0), jnp.moveaxis(val_pair, 2, 0), sink_logits.reshape(KVH, group_size), slopes))
    attended = jnp.moveaxis(per_head, 0, 2).reshape(TOKENS, QH * HEAD_DIM)
    columns = QH * HEAD_DIM // N_TP
    head_total = jnp.zeros((TOKENS, D), jnp.float32)
    for piece_id in range(N_TP):
        partial_value = jnp.dot(attended[:, piece_id * columns:(piece_id + 1) * columns], out_weight[piece_id * columns:(piece_id + 1) * columns], preferred_element_type=jnp.float32)
        head_total = head_total + lax.optimization_barrier(partial_value.astype(jnp.bfloat16)).astype(jnp.float32)
    mixed_state = (residual.astype(jnp.float32) + head_total).astype(jnp.bfloat16)
    state32 = mixed_state.astype(jnp.float32)
    normed = (state32 * lax.rsqrt(lax.optimization_barrier(jnp.mean(state32 * state32, axis=-1, keepdims=True)) + 1e-06) * norm_gain).astype(jnp.bfloat16)
    slots = N_SP * CAP
    flat_routes = routes.reshape(-1).astype(jnp.int32)
    token_of = (jnp.arange(TOKENS * TOP) // TOP).astype(jnp.int32)
    member = (flat_routes[:, None] == jnp.arange(EXPERTS)[None, :]).astype(jnp.int32)
    slot_rank = lax.optimization_barrier(jnp.sum((jnp.cumsum(member, axis=0) - 1) * member, axis=1)).astype(jnp.int32)

    def one_expert(inputs):
        expert_id, w_gate, w_up, w_down = inputs
        target = jnp.where(flat_routes == expert_id, slot_rank, slots).astype(jnp.int32)
        slot_token = jnp.zeros((slots,), jnp.int32).at[target].set(token_of, mode='drop')
        slot_rows = normed[slot_token]
        gate_pre = jnp.dot(slot_rows, w_gate, preferred_element_type=jnp.float32)
        up_pre = jnp.dot(slot_rows, w_up, preferred_element_type=jnp.float32)
        activated = (jax.nn.silu(gate_pre) * up_pre).astype(jnp.bfloat16)
        act_groups = activated.reshape(slots, N_TP, FF // N_TP).astype(jnp.float32)
        down_groups = w_down.reshape(N_TP, FF // N_TP, D).astype(jnp.float32)
        parts = jnp.einsum('mpf,pfd->pmd', act_groups, down_groups)
        parts = lax.optimization_barrier(parts.astype(jnp.bfloat16)).astype(jnp.float32)
        return lax.optimization_barrier(jnp.sum(parts, axis=0)).astype(jnp.bfloat16)
    outputs = lax.map(one_expert, (jnp.arange(EXPERTS, dtype=jnp.int32), gate_weight, up_weight, down_weight))
    flat_index = (flat_routes * slots + slot_rank).astype(jnp.int32)
    picked = outputs.reshape(EXPERTS * slots, D)[flat_index].reshape(TOKENS, TOP, D)
    expert_mix = lax.optimization_barrier(jnp.sum(route_weights[..., None] * picked.astype(jnp.float32), axis=1))
    return (state32 + expert_mix).astype(jnp.bfloat16)
```

```python
import functools

import jax
import jax.numpy as jnp
import numpy as np
from jax import lax
from jax.experimental import pallas as pl
from jax.experimental.pallas import tpu as pltpu
from jax.sharding import PartitionSpec as P

HEAD_DIM = 64
WINDOW = 128
TOP = 2
CORES = 2
F32 = jnp.float32
BF16 = jnp.bfloat16
MESH = pl.DeviceIdType.MESH


def kernel(
    S,
    T,
    slope_ref,
    sink_ref,
    q_ref,
    k_ref,
    v_ref,
    res_ref,
    gain_ref,
    routes_ref,
    rw_ref,
    wo_hbm,
    wg_hbm,
    wu_hbm,
    wd_hbm,
    out_ref,
    wo,
    wg,
    wu,
    wd,
    halo,
    att,
    pp,
    rc1,
    sb1,
    ry1,
    mixed,
    picked,
    x_all,
    xn,
    act,
    yp,
    rc2,
    sb2,
    ry2,
    rb,
    ret,
    o_all,
    w_sem,
    halo_s,
    halo_r,
    c1_s,
    c1_r,
    y1_s,
    y1_r,
    a_s,
    a_r,
    fy_s,
    fy_r,
    fc_s,
    fc_r,
    c2_s,
    c2_r,
    y2_s,
    y2_r,
    b_s,
    b_r,
    gy_s,
    gy_r,
    gc_s,
    gc_r,
):
    R, D = res_ref.shape
    Y = T // CORES
    W = D // T
    H = q_ref.shape[1] // HEAD_DIM
    KV = k_ref.shape[1] // HEAD_DIM
    G = H // KV
    C = x_all.shape[0] // S
    half = S // 2
    GM = half * C
    FL = wg.shape[1]

    me = lax.axis_index("sp")
    t = lax.axis_index("tp")
    y = t // CORES
    c = t % CORES
    oc = 1 - c

    def tp_of(yy, cc):
        return yy * CORES + cc

    def cols(tt):
        return pl.ds(pl.multiple_of(tt * W, W), W)

    def rows(s):
        return pl.ds(pl.multiple_of(s * C, C), C)

    def yo(d):
        return (y + d) % Y

    def remote(src, dst, ss, rs, **dev):
        return pltpu.make_async_remote_copy(
            src_ref=src, dst_ref=dst, send_sem=ss, recv_sem=rs, device_id=dev, device_id_type=MESH
        )

    loads = [
        pltpu.make_async_copy(wo_hbm, wo, w_sem.at[0]),
        pltpu.make_async_copy(wg_hbm.at[0], wg, w_sem.at[1]),
        pltpu.make_async_copy(wu_hbm.at[0], wu, w_sem.at[2]),
        pltpu.make_async_copy(wd_hbm.at[0], wd, w_sem.at[3]),
    ]
    for load in loads:
        load.start()

    barrier = pltpu.get_barrier_semaphore()

    @pl.loop(1, S)
    def _(d):
        pl.semaphore_signal(
            barrier, inc=1, device_id={"sp": (me + d) % S}, device_id_type=MESH
        )

    for d in range(1, Y):
        pl.semaphore_signal(
            barrier, inc=1, device_id={"tp": tp_of(yo(d), c)}, device_id_type=MESH
        )
    pl.semaphore_signal(barrier, inc=1, device_id={"tp": tp_of(y, oc)}, device_id_type=MESH)
    pl.semaphore_wait(barrier, S - 1 + Y)

    halo_copies = [
        remote(src, halo.at[i], halo_s.at[i], halo_r.at[i], sp=jnp.minimum(me + 1, S - 1))
        for i, src in enumerate((k_ref, v_ref))
    ]

    @pl.when(me < S - 1)
    def _():
        for copy in halo_copies:
            copy.start()

    r0 = routes_ref[:, 0:1]
    r1 = routes_ref[:, 1:2]
    lane_e = lax.broadcasted_iota(jnp.int32, (R, 128), 1)
    hit0 = lane_e == r0
    hit1 = lane_e == r1
    member = jnp.where(hit0 | hit1, 1.0, 0.0).astype(BF16)
    tri = jnp.where(
        lax.broadcasted_iota(jnp.int32, (R, R), 1) < lax.broadcasted_iota(jnp.int32, (R, R), 0),
        1.0,
        0.0,
    ).astype(BF16)
    rank = jnp.dot(tri, member, preferred_element_type=F32)
    rank0 = jnp.sum(jnp.where(hit0, rank, 0.0), axis=1, keepdims=True)
    rank1 = jnp.sum(jnp.where(hit1, rank, 0.0), axis=1, keepdims=True)
    slot0 = r0.astype(F32) * C + rank0
    slot1 = r1.astype(F32) * C + rank1
    lane_s = lax.broadcasted_iota(jnp.int32, (R, S * C), 1).astype(F32)

    def picker(slot):
        return jnp.where(lane_s == slot, 1.0, 0.0)

    qi = lax.broadcasted_iota(jnp.int32, (R, R), 0)
    kj = lax.broadcasted_iota(jnp.int32, (R, R), 1)
    dist_own = (qi - kj).astype(F32)
    dist_old = (qi - kj + WINDOW).astype(F32)
    nt = (((1,), (1,)), ((), ()))

    @pl.when(me > 0)
    def _():
        for copy in halo_copies:
            copy.wait_recv()

    @pl.when(me == 0)
    def _():
        halo[...] = jnp.zeros_like(halo)

    ok_own = qi >= kj
    ok_old = (kj >= qi) & (kj + me * R >= WINDOW)
    for h in range(H):
        kc = slice((h // G) * HEAD_DIM, (h // G + 1) * HEAD_DIM)
        q = q_ref[:, h * HEAD_DIM : (h + 1) * HEAD_DIM]
        slope = slope_ref[t * H + h]
        s_own = lax.dot_general(q, k_ref[:, kc], nt, preferred_element_type=F32)
        s_old = lax.dot_general(q, halo[0, :, kc], nt, preferred_element_type=F32)
        s_own = jnp.where(ok_own, s_own * HEAD_DIM**-0.5 - slope * dist_own, -jnp.inf)
        s_old = jnp.where(ok_old, s_old * HEAD_DIM**-0.5 - slope * dist_old, -jnp.inf)
        peak = jnp.maximum(
            jnp.max(s_own, axis=1, keepdims=True), jnp.max(s_old, axis=1, keepdims=True)
        )
        e_own = jnp.exp(s_own - peak)
        e_old = jnp.exp(s_old - peak)
        total = jnp.sum(e_own, axis=1, keepdims=True) + jnp.sum(e_old, axis=1, keepdims=True)
        inv = 1.0 / total
        mix = jnp.dot((e_own * inv).astype(BF16), v_ref[:, kc], preferred_element_type=F32)
        mix += jnp.dot((e_old * inv).astype(BF16), halo[1, :, kc], preferred_element_type=F32)
        keep = 1.0 / (1.0 + jnp.exp(sink_ref[h] - peak - jnp.log(total)))
        att[:, h * HEAD_DIM : (h + 1) * HEAD_DIM] = (mix * keep).astype(BF16)

    loads[0].wait()

    def project(tt):
        pp[:, cols(tt)] = jnp.dot(att[...], wo[:, cols(tt)], preferred_element_type=F32).astype(
            BF16
        )

    def c1(yy):
        return remote(
            pp.at[:, cols(tp_of(yy, oc))], rc1.at[yy], c1_s.at[yy], c1_r.at[yy], tp=tp_of(y, oc)
        )

    def y1_send(yy):
        return remote(sb1.at[yy], ry1.at[y], y1_s.at[yy], y1_r.at[y], tp=tp_of(yy, c))

    def y1_recv(yy):
        return remote(sb1.at[yy], ry1.at[yy], y1_s.at[yy], y1_r.at[yy], tp=tp_of(yy, c))

    for d in list(range(1, Y)) + [0]:
        project(tp_of(yo(d), oc))
        c1(yo(d)).start()
    for d in list(range(1, Y)) + [0]:
        project(tp_of(yo(d), c))
    for d in range(1, Y):
        c1(yo(d)).wait_recv()
        sb1[yo(d)] = (pp[:, cols(tp_of(yo(d), c))].astype(F32) + rc1[yo(d)].astype(F32)).astype(
            BF16
        )
        y1_send(yo(d)).start()
    c1(y).wait_recv()
    head_sum = pp[:, cols(t)].astype(F32) + rc1[y].astype(F32)
    for d in range(1, Y):
        y1_recv(yo(d)).wait_recv()
        head_sum = head_sum + ry1[yo(d)].astype(F32)
    mixed[...] = (res_ref[:, cols(t)].astype(F32) + head_sum).astype(BF16)

    both = (picker(slot0) + picker(slot1)).T.astype(BF16)
    picked[...] = jnp.dot(both, mixed[...], preferred_element_type=F32).astype(BF16)

    loc = me % half
    near = (me // half) * half
    far = half - near

    def place(base, d):
        return base + (loc + half - d) % half

    def a_send(e):
        return remote(
            picked.at[rows(e)], x_all.at[rows(me), cols(t)], a_s.at[e], a_r.at[me], sp=e
        )

    def a_recv(s):
        return remote(picked.at[rows(s)], x_all.at[rows(s), cols(t)], a_s.at[s], a_r.at[s], sp=s)

    def fy_send(s, yy):
        ref = x_all.at[rows(s), cols(t)]
        return remote(ref, ref, fy_s.at[s, yy], fy_r.at[s, y], tp=tp_of(yy, c))

    def fy_recv(s, yy):
        ref = x_all.at[rows(s), cols(tp_of(yy, c))]
        return remote(ref, ref, fy_s.at[s, yy], fy_r.at[s, yy], tp=tp_of(yy, c))

    def fc_send(s, yy):
        ref = x_all.at[rows(s), cols(tp_of(yy, c))]
        return remote(ref, ref, fc_s.at[s, yy], fc_r.at[s, yy], tp=tp_of(y, oc))

    def fc_recv(s, yy):
        ref = x_all.at[rows(s), cols(tp_of(yy, oc))]
        return remote(ref, ref, fc_s.at[s, yy], fc_r.at[s, yy], tp=tp_of(y, oc))

    @pl.loop(1, half)
    def _(d):
        a_send(near + (loc + d) % half).start()

    @pl.loop(0, half)
    def _(d):
        a_send(far + (loc + d) % half).start()

    x_all[rows(me), cols(t)] = picked[rows(me)]

    def forward(s):
        for d in range(1, Y):
            fy_send(s, yo(d)).start()
        fc_send(s, y).start()

    def forward_group(base, first):
        @pl.loop(first, half)
        def _(d):
            s = place(base, d)
            a_recv(s).wait_recv()
            forward(s)

    def relay_group(base):
        @pl.loop(0, half)
        def _(d):
            s = place(base, d)
            for i in range(1, Y):
                fy_recv(s, yo(i)).wait_recv()
                fc_send(s, yo(i)).start()

    def norm_group(base):
        @pl.loop(0, half)
        def _(d):
            s = place(base, d)
            for i in range(Y):
                fc_recv(s, yo(i)).wait_recv()
            x = x_all[rows(s)].astype(F32)
            scale = lax.rsqrt(jnp.mean(x * x, axis=1, keepdims=True) + 1e-06)
            xn[rows(s)] = (x * scale * gain_ref[...]).astype(BF16)

    TN = min(256, FL)

    def hidden_group(base):
        at = pl.ds(pl.multiple_of(base * C, C), GM)

        @pl.loop(0, FL // TN)
        def _(n):
            nn = pl.ds(pl.multiple_of(n * TN, TN), TN)
            gate = jnp.dot(xn[at], wg[:, nn], preferred_element_type=F32)
            up = jnp.dot(xn[at], wu[:, nn], preferred_element_type=F32)
            act[:, nn] = (gate / (1.0 + jnp.exp(-gate)) * up).astype(BF16)

    def c2(g, yy):
        return remote(
            yp.at[g, :, cols(tp_of(yy, oc))],
            rc2.at[g, yy],
            c2_s.at[g, yy],
            c2_r.at[g, yy],
            tp=tp_of(y, oc),
        )

    def down_block(g, tt):
        yp[g, :, cols(tt)] = jnp.dot(act[...], wd[:, cols(tt)], preferred_element_type=F32).astype(
            BF16
        )

    def down_group(g):
        @pl.loop(0, Y)
        def _(d):
            yy = yo(d + 1)
            down_block(g, tp_of(yy, oc))
            c2(g, yy).start()

        @pl.loop(0, Y)
        def _(d):
            down_block(g, tp_of(yo(d + 1), c))

    def y2_send(g, p, yy):
        return remote(
            sb2.at[g, yy, rows(p)],
            ry2.at[g, y, rows(p)],
            y2_s.at[g, p, yy],
            y2_r.at[g, p, y],
            tp=tp_of(yy, c),
        )

    def y2_recv(g, p, yy):
        return remote(
            sb2.at[g, yy, rows(p)],
            ry2.at[g, yy, rows(p)],
            y2_s.at[g, p, yy],
            y2_r.at[g, p, yy],
            tp=tp_of(yy, c),
        )

    def b_send(s):
        return remote(rb.at[rows(s)], ret.at[rows(me)], b_s.at[s], b_r.at[me], sp=s)

    def b_recv(s):
        return remote(rb.at[rows(s)], ret.at[rows(s)], b_s.at[s], b_r.at[s], sp=s)

    def pair_sum(g):
        for d in list(range(1, Y)) + [0]:
            yy = yo(d)
            c2(g, yy).wait_recv()

            @pl.loop(0, half)
            def _(i):
                p = (loc + half - i) % half
                sb2[g, yy, rows(p)] = (
                    yp[g, rows(p), cols(tp_of(yy, c))].astype(F32) + rc2[g, yy, rows(p)].astype(F32)
                ).astype(BF16)
                if d:
                    y2_send(g, p, yy).start()

    def send_back(g, base):
        @pl.loop(0, half)
        def _(i):
            p = (loc + half - i) % half
            s = base + p
            total = sb2[g, y, rows(p)].astype(F32)
            for d in range(1, Y):
                y2_recv(g, p, yo(d)).wait_recv()
                total = total + ry2[g, yo(d), rows(p)].astype(F32)
            rb[rows(s)] = total.astype(BF16)

            @pl.when(s != me)
            def _():
                b_send(s).start()

    forward(me)
    forward_group(near, 1)
    relay_group(near)
    norm_group(near)
    loads[1].wait()
    loads[2].wait()
    hidden_group(near)
    loads[3].wait()
    down_group(0)
    forward_group(far, 0)
    pair_sum(0)
    relay_group(far)
    norm_group(far)
    hidden_group(far)
    send_back(0, near)
    down_group(1)
    pair_sum(1)
    send_back(1, far)

    ret[rows(me)] = rb[rows(me)]

    @pl.loop(1, S)
    def _(d):
        b_recv((me + d) % S).wait_recv()

    mix0 = jnp.dot(picker(slot0).astype(BF16), ret[...], preferred_element_type=F32)
    mix1 = jnp.dot(picker(slot1).astype(BF16), ret[...], preferred_element_type=F32)
    o_all[:, cols(t)] = (
        mixed[...].astype(F32) + (rw_ref[:, 0:1] * mix0 + rw_ref[:, 1:2] * mix1)
    ).astype(BF16)

    def gy_send(yy):
        ref = o_all.at[:, cols(t)]
        return remote(ref, ref, gy_s.at[yy], gy_r.at[y], tp=tp_of(yy, c))

    def gy_recv(yy):
        ref = o_all.at[:, cols(tp_of(yy, c))]
        return remote(ref, ref, gy_s.at[yy], gy_r.at[yy], tp=tp_of(yy, c))

    def gc_send(yy):
        ref = o_all.at[:, cols(tp_of(yy, c))]
        return remote(ref, ref, gc_s.at[yy], gc_r.at[yy], tp=tp_of(y, oc))

    def gc_recv(yy):
        ref = o_all.at[:, cols(tp_of(yy, oc))]
        return remote(ref, ref, gc_s.at[yy], gc_r.at[yy], tp=tp_of(y, oc))

    for d in range(1, Y):
        gy_send(yo(d)).start()
    gc_send(y).start()
    for d in range(1, Y):
        gy_recv(yo(d)).wait_recv()
        gc_send(yo(d)).start()
    for d in range(Y):
        gc_recv(yo(d)).wait_recv()
    out_ref[...] = o_all[...]

    @pl.when(me < S - 1)
    def _():
        for copy in halo_copies:
            copy.wait_send()

    for d in range(Y):
        c1(yo(d)).wait_send()
        gc_send(yo(d)).wait_send()
        for g in range(2):
            c2(g, yo(d)).wait_send()
    for d in range(1, Y):
        y1_send(yo(d)).wait_send()
        gy_send(yo(d)).wait_send()

    @pl.loop(1, S)
    def _(d):
        a_send((me + d) % S).wait_send()
        b_send((me + d) % S).wait_send()

    @pl.loop(0, S)
    def _(s):
        for d in range(Y):
            fc_send(s, yo(d)).wait_send()
        for d in range(1, Y):
            fy_send(s, yo(d)).wait_send()

    @pl.loop(0, half)
    def _(p):
        for d in range(1, Y):
            for g in range(2):
                y2_send(g, p, yo(d)).wait_send()


def per_device(
    S,
    T,
    queries,
    key_rows,
    value_rows,
    sink_logits,
    out_weight,
    residual,
    norm_gain,
    routes,
    route_weights,
    gate_weight,
    up_weight,
    down_weight,
):
    R, D = residual.shape
    HW = queries.shape[1]
    heads = HW // HEAD_DIM * T
    Y = T // CORES
    W = D // T
    C = 2 * R * TOP // S
    half = S // 2
    GM = half * C
    FL = gate_weight.shape[2]
    slopes = jnp.asarray(np.exp2(-8.0 * np.arange(1, heads + 1) / heads).astype(np.float32))
    vmem = pl.BlockSpec(memory_space=pltpu.VMEM)
    smem = pl.BlockSpec(memory_space=pltpu.SMEM)
    hbm = pl.BlockSpec(memory_space=pl.ANY)
    dma = pltpu.SemaphoreType.DMA
    v = pltpu.VMEM
    return pl.pallas_call(
        functools.partial(kernel, S, T),
        out_shape=jax.ShapeDtypeStruct((R, D), BF16),
        in_specs=[smem, smem] + [vmem] * 7 + [hbm] * 4,
        out_specs=vmem,
        scratch_shapes=[
            v(out_weight.shape, BF16),
            v(gate_weight.shape[1:], BF16),
            v(up_weight.shape[1:], BF16),
            v(down_weight.shape[1:], BF16),
            v((2,) + key_rows.shape, BF16),
            v((R, HW), BF16),
            v((R, D), BF16),
            v((Y, R, W), BF16),
            v((Y, R, W), BF16),
            v((Y, R, W), BF16),
            v((R, W), BF16),
            v((S * C, W), BF16),
            v((S * C, D), BF16),
            v((S * C, D), BF16),
            v((GM, FL), BF16),
            v((2, GM, D), BF16),
            v((2, Y, GM, W), BF16),
            v((2, Y, GM, W), BF16),
            v((2, Y, GM, W), BF16),
            v((S * C, W), BF16),
            v((S * C, W), BF16),
            v((R, D), BF16),
            dma((4,)),
            dma((2,)),
            dma((2,)),
            dma((Y,)),
            dma((Y,)),
            dma((Y,)),
            dma((Y,)),
            dma((S,)),
            dma((S,)),
            dma((S, Y)),
            dma((S, Y)),
            dma((S, Y)),
            dma((S, Y)),
            dma((2, Y)),
            dma((2, Y)),
            dma((2, half, Y)),
            dma((2, half, Y)),
            dma((S,)),
            dma((S,)),
            dma((Y,)),
            dma((Y,)),
            dma((Y,)),
            dma((Y,)),
        ],
        compiler_params=pltpu.CompilerParams(
            collective_id=0, has_side_effects=True, vmem_limit_bytes=60 * 1024 * 1024
        ),
        name="layer",
    )(
        slopes,
        sink_logits,
        queries,
        key_rows,
        value_rows,
        residual,
        norm_gain.reshape(1, D),
        routes,
        route_weights,
        out_weight,
        gate_weight,
        up_weight,
        down_weight,
    )


def solution(mesh):
    placed = (
        P("sp", "tp"),
        P("sp", "tp"),
        P("sp", "tp"),
        P("tp"),
        P("tp", None),
        P("sp", None),
        P(),
        P("sp", None),
        P("sp", None),
        P("sp", None, "tp"),
        P("sp", None, "tp"),
        P("sp", "tp", None),
    )
    return jax.shard_map(
        functools.partial(per_device, mesh.shape["sp"], mesh.shape["tp"]),
        mesh=mesh,
        in_specs=placed,
        out_specs=P("sp", None),
        check_vma=False,
    )
```

```python
import functools

import jax
import jax.numpy as jnp
import numpy as np
from jax import lax
from jax.experimental import pallas as pl
from jax.experimental.pallas import tpu as pltpu
from jax.sharding import PartitionSpec as P

HEAD_DIM = 64
WINDOW = 128
TOP = 2
CORES = 2
F32 = jnp.float32
BF16 = jnp.bfloat16
MESH = pl.DeviceIdType.MESH


def kernel(
    S,
    T,
    slope_ref,
    sink_ref,
    q_ref,
    k_ref,
    v_ref,
    res_ref,
    gain_ref,
    routes_ref,
    rw_ref,
    wo_hbm,
    wg_hbm,
    wu_hbm,
    wd_hbm,
    out_ref,
    wo,
    wg,
    wu,
    wd,
    halo,
    att,
    pp,
    rc1,
    sb1,
    ry1,
    mixed,
    picked,
    x_all,
    xn,
    act,
    yp,
    rc2,
    sb2,
    ry2,
    rb,
    ret,
    o_all,
    w_sem,
    halo_s,
    halo_r,
    c1_s,
    c1_r,
    y1_s,
    y1_r,
    a_s,
    a_r,
    fy_s,
    fy_r,
    fc_s,
    fc_r,
    c2_s,
    c2_r,
    y2_s,
    y2_r,
    b_s,
    b_r,
    gy_s,
    gy_r,
    gc_s,
    gc_r,
):
    R, D = res_ref.shape
    Y = T // CORES
    W = D // T
    H = q_ref.shape[1] // HEAD_DIM
    KV = k_ref.shape[1] // HEAD_DIM
    G = H // KV
    C = x_all.shape[0] // S
    half = S // 2
    GM = half * C
    FL = wg.shape[1]

    me = lax.axis_index("sp")
    t = lax.axis_index("tp")
    y = t // CORES
    c = t % CORES
    oc = 1 - c

    def tp_of(yy, cc):
        return yy * CORES + cc

    def cols(tt):
        return pl.ds(pl.multiple_of(tt * W, W), W)

    def rows(s):
        return pl.ds(pl.multiple_of(s * C, C), C)

    def yo(d):
        return (y + d) % Y

    def remote(src, dst, ss, rs, **dev):
        return pltpu.make_async_remote_copy(
            src_ref=src, dst_ref=dst, send_sem=ss, recv_sem=rs, device_id=dev, device_id_type=MESH
        )

    loads = [
        pltpu.make_async_copy(wo_hbm, wo, w_sem.at[0]),
        pltpu.make_async_copy(wg_hbm.at[0], wg, w_sem.at[1]),
        pltpu.make_async_copy(wu_hbm.at[0], wu, w_sem.at[2]),
        pltpu.make_async_copy(wd_hbm.at[0], wd, w_sem.at[3]),
    ]
    for load in loads:
        load.start()

    barrier = pltpu.get_barrier_semaphore()

    @pl.loop(1, S)
    def _(d):
        pl.semaphore_signal(
            barrier, inc=1, device_id={"sp": (me + d) % S}, device_id_type=MESH
        )

    for d in range(1, Y):
        pl.semaphore_signal(
            barrier, inc=1, device_id={"tp": tp_of(yo(d), c)}, device_id_type=MESH
        )
    pl.semaphore_signal(barrier, inc=1, device_id={"tp": tp_of(y, oc)}, device_id_type=MESH)
    pl.semaphore_wait(barrier, S - 1 + Y)

    halo_copies = [
        remote(src, halo.at[i], halo_s.at[i], halo_r.at[i], sp=jnp.minimum(me + 1, S - 1))
        for i, src in enumerate((k_ref, v_ref))
    ]

    @pl.when(me < S - 1)
    def _():
        for copy in halo_copies:
            copy.start()

    def column(row):
        return jnp.broadcast_to(row, (R, R)).T[:, 0:1]

    r0 = column(routes_ref[0:1, :].astype(F32)).astype(jnp.int32)
    r1 = column(routes_ref[1:2, :].astype(F32)).astype(jnp.int32)
    lane_e = lax.broadcasted_iota(jnp.int32, (R, 128), 1)
    hit0 = lane_e == r0
    hit1 = lane_e == r1
    member = jnp.where(hit0 | hit1, 1.0, 0.0).astype(BF16)
    tri = jnp.where(
        lax.broadcasted_iota(jnp.int32, (R, R), 1) < lax.broadcasted_iota(jnp.int32, (R, R), 0),
        1.0,
        0.0,
    ).astype(BF16)
    rank = jnp.dot(tri, member, preferred_element_type=F32)
    rank0 = jnp.sum(jnp.where(hit0, rank, 0.0), axis=1, keepdims=True)
    rank1 = jnp.sum(jnp.where(hit1, rank, 0.0), axis=1, keepdims=True)
    slot0 = r0.astype(F32) * C + rank0
    slot1 = r1.astype(F32) * C + rank1
    lane_s = lax.broadcasted_iota(jnp.int32, (R, S * C), 1).astype(F32)

    def picker(slot):
        return jnp.where(lane_s == slot, 1.0, 0.0)

    qi = lax.broadcasted_iota(jnp.int32, (R, R), 0)
    kj = lax.broadcasted_iota(jnp.int32, (R, R), 1)
    dist_own = (qi - kj).astype(F32)
    dist_old = (qi - kj + WINDOW).astype(F32)
    nt = (((1,), (1,)), ((), ()))

    ok_own = qi >= kj
    ok_old = (kj >= qi) & (kj + me * R >= WINDOW)

    def head(h):
        return slice(h * HEAD_DIM, (h + 1) * HEAD_DIM), slice(
            (h // G) * HEAD_DIM, (h // G + 1) * HEAD_DIM
        )

    def scores(h, keys, dist, ok):
        raw = lax.dot_general(q_ref[:, head(h)[0]], keys, nt, preferred_element_type=F32)
        return jnp.where(ok, raw * HEAD_DIM**-0.5 - slope_ref[t * H + h] * dist, -jnp.inf)

    own = [scores(h, k_ref[:, head(h)[1]], dist_own, ok_own) for h in range(H)]
    own_peak = [jnp.max(x, axis=1, keepdims=True) for x in own]

    @pl.when(me > 0)
    def _():
        for copy in halo_copies:
            copy.wait_recv()

    @pl.when(me == 0)
    def _():
        halo[...] = jnp.zeros_like(halo)

    for h in range(H):
        hc, kc = head(h)
        s_own = own[h]
        s_old = scores(h, halo[0, :, kc], dist_old, ok_old)
        peak = jnp.maximum(own_peak[h], jnp.max(s_old, axis=1, keepdims=True))
        e_own = jnp.exp(s_own - peak)
        e_old = jnp.exp(s_old - peak)
        total = jnp.sum(e_own, axis=1, keepdims=True) + jnp.sum(e_old, axis=1, keepdims=True)
        inv = 1.0 / total
        mix = jnp.dot((e_own * inv).astype(BF16), v_ref[:, kc], preferred_element_type=F32)
        mix += jnp.dot((e_old * inv).astype(BF16), halo[1, :, kc], preferred_element_type=F32)
        keep = 1.0 / (1.0 + jnp.exp(sink_ref[h] - peak - jnp.log(total)))
        att[:, hc] = (mix * keep).astype(BF16)

    loads[0].wait()

    def project(tt):
        pp[:, cols(tt)] = jnp.dot(att[...], wo[:, cols(tt)], preferred_element_type=F32).astype(
            BF16
        )

    def c1(yy):
        return remote(
            pp.at[:, cols(tp_of(yy, oc))], rc1.at[yy], c1_s.at[yy], c1_r.at[yy], tp=tp_of(y, oc)
        )

    def y1_send(yy):
        return remote(sb1.at[yy], ry1.at[y], y1_s.at[yy], y1_r.at[y], tp=tp_of(yy, c))

    def y1_recv(yy):
        return remote(sb1.at[yy], ry1.at[yy], y1_s.at[yy], y1_r.at[yy], tp=tp_of(yy, c))

    for d in list(range(1, Y)) + [0]:
        project(tp_of(yo(d), oc))
        c1(yo(d)).start()
    for d in list(range(1, Y)) + [0]:
        project(tp_of(yo(d), c))
    for d in range(1, Y):
        c1(yo(d)).wait_recv()
        sb1[yo(d)] = (pp[:, cols(tp_of(yo(d), c))].astype(F32) + rc1[yo(d)].astype(F32)).astype(
            BF16
        )
        y1_send(yo(d)).start()
    c1(y).wait_recv()
    head_sum = pp[:, cols(t)].astype(F32) + rc1[y].astype(F32)
    for d in range(1, Y):
        y1_recv(yo(d)).wait_recv()
        head_sum = head_sum + ry1[yo(d)].astype(F32)
    mixed[...] = (res_ref[:, cols(t)].astype(F32) + head_sum).astype(BF16)

    both = (picker(slot0) + picker(slot1)).T.astype(BF16)
    picked[...] = jnp.dot(both, mixed[...], preferred_element_type=F32).astype(BF16)

    loc = me // 2
    near = me % 2
    far = 1 - near

    def source(par, p):
        return 2 * p + par

    def place(par, d):
        return source(par, (loc + half - d) % half)

    def spot(s):
        return rows((s % 2) * half + s // 2)

    def a_send(e):
        return remote(
            picked.at[rows(e)], x_all.at[spot(me), cols(t)], a_s.at[e], a_r.at[me], sp=e
        )

    def a_recv(s):
        return remote(picked.at[rows(s)], x_all.at[spot(s), cols(t)], a_s.at[s], a_r.at[s], sp=s)

    def fy_send(s, yy):
        ref = x_all.at[spot(s), cols(t)]
        return remote(ref, ref, fy_s.at[s, yy], fy_r.at[s, y], tp=tp_of(yy, c))

    def fy_recv(s, yy):
        ref = x_all.at[spot(s), cols(tp_of(yy, c))]
        return remote(ref, ref, fy_s.at[s, yy], fy_r.at[s, yy], tp=tp_of(yy, c))

    def fc_send(s, yy):
        ref = x_all.at[spot(s), cols(tp_of(yy, c))]
        return remote(ref, ref, fc_s.at[s, yy], fc_r.at[s, yy], tp=tp_of(y, oc))

    def fc_recv(s, yy):
        ref = x_all.at[spot(s), cols(tp_of(yy, oc))]
        return remote(ref, ref, fc_s.at[s, yy], fc_r.at[s, yy], tp=tp_of(y, oc))

    @pl.loop(1, half)
    def _(d):
        a_send(source(near, (loc + d) % half)).start()

    @pl.loop(0, half)
    def _(d):
        a_send(source(far, (loc + d) % half)).start()

    x_all[spot(me), cols(t)] = picked[rows(me)]

    def forward(s):
        for d in range(1, Y):
            fy_send(s, yo(d)).start()
        fc_send(s, y).start()

    def relay(s):
        for i in range(1, Y):
            fy_recv(s, yo(i)).wait_recv()
            fc_send(s, yo(i)).start()

    def arrive(s):
        a_recv(s).wait_recv()
        forward(s)

    def norm_group(base):
        @pl.loop(0, half)
        def _(d):
            s = place(base, d)
            for i in range(Y):
                fc_recv(s, yo(i)).wait_recv()
            x = x_all[spot(s)].astype(F32)
            scale = lax.rsqrt(jnp.mean(x * x, axis=1, keepdims=True) + 1e-06)
            xn[spot(s)] = (x * scale * gain_ref[...]).astype(BF16)

    TN = min(256, FL)

    def hidden_group(base):
        at = pl.ds(pl.multiple_of(base * GM, GM), GM)

        @pl.loop(0, FL // TN)
        def _(n):
            nn = pl.ds(pl.multiple_of(n * TN, TN), TN)
            gate = jnp.dot(xn[at], wg[:, nn], preferred_element_type=F32)
            up = jnp.dot(xn[at], wu[:, nn], preferred_element_type=F32)
            act[:, nn] = (gate / (1.0 + jnp.exp(-gate)) * up).astype(BF16)

    def c2(g, yy):
        return remote(
            yp.at[g, :, cols(tp_of(yy, oc))],
            rc2.at[g, yy],
            c2_s.at[g, yy],
            c2_r.at[g, yy],
            tp=tp_of(y, oc),
        )

    def down_block(g, tt):
        yp[g, :, cols(tt)] = jnp.dot(act[...], wd[:, cols(tt)], preferred_element_type=F32).astype(
            BF16
        )

    def down_group(g):
        @pl.loop(0, Y)
        def _(d):
            yy = yo(d + 1)
            down_block(g, tp_of(yy, oc))
            c2(g, yy).start()

        @pl.loop(0, Y)
        def _(d):
            down_block(g, tp_of(yo(d + 1), c))

    def y2_send(g, p, yy):
        return remote(
            sb2.at[g, yy, rows(p)],
            ry2.at[g, y, rows(p)],
            y2_s.at[g, p, yy],
            y2_r.at[g, p, y],
            tp=tp_of(yy, c),
        )

    def y2_recv(g, p, yy):
        return remote(
            sb2.at[g, yy, rows(p)],
            ry2.at[g, yy, rows(p)],
            y2_s.at[g, p, yy],
            y2_r.at[g, p, yy],
            tp=tp_of(yy, c),
        )

    def b_send(s):
        return remote(rb.at[rows(s)], ret.at[rows(me)], b_s.at[s], b_r.at[me], sp=s)

    def b_recv(s):
        return remote(rb.at[rows(s)], ret.at[rows(s)], b_s.at[s], b_r.at[s], sp=s)

    def pair_sum(g):
        for d in list(range(1, Y)) + [0]:
            yy = yo(d)
            c2(g, yy).wait_recv()

            @pl.loop(0, half)
            def _(i):
                p = (loc + half - i) % half
                sb2[g, yy, rows(p)] = (
                    yp[g, rows(p), cols(tp_of(yy, c))].astype(F32) + rc2[g, yy, rows(p)].astype(F32)
                ).astype(BF16)
                if d:
                    y2_send(g, p, yy).start()

    def send_back(g, base):
        @pl.loop(0, half)
        def _(i):
            p = (loc + half - i) % half
            s = source(base, p)
            total = sb2[g, y, rows(p)].astype(F32)
            for d in range(1, Y):
                y2_recv(g, p, yo(d)).wait_recv()
                total = total + ry2[g, yo(d), rows(p)].astype(F32)
            rb[rows(s)] = total.astype(BF16)

            @pl.when(s != me)
            def _():
                b_send(s).start()

    forward(me)

    @pl.loop(1, half)
    def _(d):
        arrive(place(near, d))

    @pl.loop(0, half)
    def _(d):
        relay(place(near, d))
        arrive(place(far, d))

    norm_group(near)
    loads[1].wait()
    loads[2].wait()
    hidden_group(near)

    @pl.loop(0, half)
    def _(d):
        relay(place(far, d))

    loads[3].wait()
    down_group(0)
    norm_group(far)
    pair_sum(0)
    hidden_group(far)
    send_back(0, near)
    down_group(1)
    pair_sum(1)
    send_back(1, far)

    ret[rows(me)] = rb[rows(me)]

    @pl.loop(1, S)
    def _(d):
        b_recv((me + d) % S).wait_recv()

    mix0 = jnp.dot(picker(slot0).astype(BF16), ret[...], preferred_element_type=F32)
    mix1 = jnp.dot(picker(slot1).astype(BF16), ret[...], preferred_element_type=F32)
    o_all[:, cols(t)] = (
        mixed[...].astype(F32) + (column(rw_ref[0:1, :]) * mix0 + column(rw_ref[1:2, :]) * mix1)
    ).astype(BF16)

    def gy_send(yy):
        ref = o_all.at[:, cols(t)]
        return remote(ref, ref, gy_s.at[yy], gy_r.at[y], tp=tp_of(yy, c))

    def gy_recv(yy):
        ref = o_all.at[:, cols(tp_of(yy, c))]
        return remote(ref, ref, gy_s.at[yy], gy_r.at[yy], tp=tp_of(yy, c))

    def gc_send(yy):
        ref = o_all.at[:, cols(tp_of(yy, c))]
        return remote(ref, ref, gc_s.at[yy], gc_r.at[yy], tp=tp_of(y, oc))

    def gc_recv(yy):
        ref = o_all.at[:, cols(tp_of(yy, oc))]
        return remote(ref, ref, gc_s.at[yy], gc_r.at[yy], tp=tp_of(y, oc))

    for d in range(1, Y):
        gy_send(yo(d)).start()
    gc_send(y).start()
    for d in range(1, Y):
        gy_recv(yo(d)).wait_recv()
        gc_send(yo(d)).start()
    for d in range(Y):
        gc_recv(yo(d)).wait_recv()
    out_ref[...] = o_all[...]

    @pl.when(me < S - 1)
    def _():
        for copy in halo_copies:
            copy.wait_send()

    for d in range(Y):
        c1(yo(d)).wait_send()
        gc_send(yo(d)).wait_send()
        for g in range(2):
            c2(g, yo(d)).wait_send()
    for d in range(1, Y):
        y1_send(yo(d)).wait_send()
        gy_send(yo(d)).wait_send()

    @pl.loop(1, S)
    def _(d):
        a_send((me + d) % S).wait_send()
        b_send((me + d) % S).wait_send()

    @pl.loop(0, S)
    def _(s):
        for d in range(Y):
            fc_send(s, yo(d)).wait_send()
        for d in range(1, Y):
            fy_send(s, yo(d)).wait_send()

    @pl.loop(0, half)
    def _(p):
        for d in range(1, Y):
            for g in range(2):
                y2_send(g, p, yo(d)).wait_send()


def per_device(
    S,
    T,
    queries,
    key_rows,
    value_rows,
    sink_logits,
    out_weight,
    residual,
    norm_gain,
    routes,
    route_weights,
    gate_weight,
    up_weight,
    down_weight,
):
    R, D = residual.shape
    HW = queries.shape[1]
    heads = HW // HEAD_DIM * T
    Y = T // CORES
    W = D // T
    C = 2 * R * TOP // S
    half = S // 2
    GM = half * C
    FL = gate_weight.shape[2]
    slopes = jnp.asarray(np.exp2(-8.0 * np.arange(1, heads + 1) / heads).astype(np.float32))
    vmem = pl.BlockSpec(memory_space=pltpu.VMEM)
    smem = pl.BlockSpec(memory_space=pltpu.SMEM)
    hbm = pl.BlockSpec(memory_space=pl.ANY)
    dma = pltpu.SemaphoreType.DMA
    v = pltpu.VMEM
    return pl.pallas_call(
        functools.partial(kernel, S, T),
        out_shape=jax.ShapeDtypeStruct((R, D), BF16),
        in_specs=[smem, smem] + [vmem] * 7 + [hbm] * 4,
        out_specs=vmem,
        scratch_shapes=[
            v(out_weight.shape, BF16),
            v(gate_weight.shape[1:], BF16),
            v(up_weight.shape[1:], BF16),
            v(down_weight.shape[1:], BF16),
            v((2,) + key_rows.shape, BF16),
            v((R, HW), BF16),
            v((R, D), BF16),
            v((Y, R, W), BF16),
            v((Y, R, W), BF16),
            v((Y, R, W), BF16),
            v((R, W), BF16),
            v((S * C, W), BF16),
            v((S * C, D), BF16),
            v((S * C, D), BF16),
            v((GM, FL), BF16),
            v((2, GM, D), BF16),
            v((2, Y, GM, W), BF16),
            v((2, Y, GM, W), BF16),
            v((2, Y, GM, W), BF16),
            v((S * C, W), BF16),
            v((S * C, W), BF16),
            v((R, D), BF16),
            dma((4,)),
            dma((2,)),
            dma((2,)),
            dma((Y,)),
            dma((Y,)),
            dma((Y,)),
            dma((Y,)),
            dma((S,)),
            dma((S,)),
            dma((S, Y)),
            dma((S, Y)),
            dma((S, Y)),
            dma((S, Y)),
            dma((2, Y)),
            dma((2, Y)),
            dma((2, half, Y)),
            dma((2, half, Y)),
            dma((S,)),
            dma((S,)),
            dma((Y,)),
            dma((Y,)),
            dma((Y,)),
            dma((Y,)),
        ],
        compiler_params=pltpu.CompilerParams(
            collective_id=0, has_side_effects=True, vmem_limit_bytes=60 * 1024 * 1024
        ),
        name="layer",
    )(
        slopes,
        sink_logits,
        queries,
        key_rows,
        value_rows,
        residual,
        norm_gain.reshape(1, D),
        routes.T,
        route_weights.T,
        out_weight,
        gate_weight,
        up_weight,
        down_weight,
    )


def solution(mesh):
    placed = (
        P("sp", "tp"),
        P("sp", "tp"),
        P("sp", "tp"),
        P("tp"),
        P("tp", None),
        P("sp", None),
        P(),
        P("sp", None),
        P("sp", None),
        P("sp", None, "tp"),
        P("sp", None, "tp"),
        P("sp", "tp", None),
    )
    return jax.shard_map(
        functools.partial(per_device, mesh.shape["sp"], mesh.shape["tp"]),
        mesh=mesh,
        in_specs=placed,
        out_specs=P("sp", None),
        check_vma=False,
    )
```

```python
import functools

import jax
import jax.numpy as jnp
import numpy as np
from jax import lax
from jax.experimental import pallas as pl
from jax.experimental.pallas import tpu as pltpu
from jax.sharding import PartitionSpec as P

HEAD_DIM = 64
WINDOW = 128
TOP = 2
CORES = 2
F32 = jnp.float32
BF16 = jnp.bfloat16
MESH = pl.DeviceIdType.MESH


def kernel(
    S,
    T,
    slope_ref,
    sink_ref,
    q_ref,
    k_ref,
    v_ref,
    res_ref,
    gain_ref,
    routes_ref,
    rw_ref,
    wo_hbm,
    wg_hbm,
    wu_hbm,
    wd_hbm,
    out_ref,
    wo,
    wg,
    wu,
    wd,
    halo,
    att,
    pp,
    rc1,
    sb1,
    ry1,
    mixed,
    picked,
    x_all,
    xn,
    act,
    yp,
    rc2,
    sb2,
    ry2,
    rb,
    ret,
    o_all,
    w_sem,
    halo_s,
    halo_r,
    c1_s,
    c1_r,
    y1_s,
    y1_r,
    a_s,
    a_r,
    fy_s,
    fy_r,
    fc_s,
    fc_r,
    c2_s,
    c2_r,
    y2_s,
    y2_r,
    b_s,
    b_r,
    gy_s,
    gy_r,
    gc_s,
    gc_r,
):
    R, D = res_ref.shape
    Y = T // CORES
    W = D // T
    H = q_ref.shape[1] // HEAD_DIM
    KV = k_ref.shape[1] // HEAD_DIM
    G = H // KV
    C = x_all.shape[0] // S
    half = S // 2
    GM = half * C
    FL = wg.shape[1]

    me = lax.axis_index("sp")
    t = lax.axis_index("tp")
    y = t // CORES
    c = t % CORES
    oc = 1 - c

    def tp_of(yy, cc):
        return yy * CORES + cc

    def cols(tt):
        return pl.ds(pl.multiple_of(tt * W, W), W)

    def rows(s):
        return pl.ds(pl.multiple_of(s * C, C), C)

    def yo(d):
        return (y + d) % Y

    def remote(src, dst, ss, rs, **dev):
        return pltpu.make_async_remote_copy(
            src_ref=src, dst_ref=dst, send_sem=ss, recv_sem=rs, device_id=dev, device_id_type=MESH
        )

    loads = [
        pltpu.make_async_copy(wo_hbm, wo, w_sem.at[0]),
        pltpu.make_async_copy(wg_hbm.at[0], wg, w_sem.at[1]),
        pltpu.make_async_copy(wu_hbm.at[0], wu, w_sem.at[2]),
        pltpu.make_async_copy(wd_hbm.at[0], wd, w_sem.at[3]),
    ]
    for load in loads:
        load.start()

    barrier = pltpu.get_barrier_semaphore()

    @pl.loop(1, S)
    def _(d):
        pl.semaphore_signal(
            barrier, inc=1, device_id={"sp": (me + d) % S}, device_id_type=MESH
        )

    for d in range(1, Y):
        pl.semaphore_signal(
            barrier, inc=1, device_id={"tp": tp_of(yo(d), c)}, device_id_type=MESH
        )
    pl.semaphore_signal(barrier, inc=1, device_id={"tp": tp_of(y, oc)}, device_id_type=MESH)
    pl.semaphore_wait(barrier, S - 1 + Y)

    halo_copies = [
        remote(src, halo.at[i], halo_s.at[i], halo_r.at[i], sp=jnp.minimum(me + 1, S - 1))
        for i, src in enumerate((k_ref, v_ref))
    ]

    @pl.when(me < S - 1)
    def _():
        for copy in halo_copies:
            copy.start()

    def column(row):
        return jnp.broadcast_to(row, (R, R)).T[:, 0:1]

    r0 = column(routes_ref[0:1, :].astype(F32)).astype(jnp.int32)
    r1 = column(routes_ref[1:2, :].astype(F32)).astype(jnp.int32)
    lane_e = lax.broadcasted_iota(jnp.int32, (R, 128), 1)
    hit0 = lane_e == r0
    hit1 = lane_e == r1
    member = jnp.where(hit0 | hit1, 1.0, 0.0).astype(BF16)
    tri = jnp.where(
        lax.broadcasted_iota(jnp.int32, (R, R), 1) < lax.broadcasted_iota(jnp.int32, (R, R), 0),
        1.0,
        0.0,
    ).astype(BF16)
    rank = jnp.dot(tri, member, preferred_element_type=F32)
    rank0 = jnp.sum(jnp.where(hit0, rank, 0.0), axis=1, keepdims=True)
    rank1 = jnp.sum(jnp.where(hit1, rank, 0.0), axis=1, keepdims=True)
    slot0 = r0.astype(F32) * C + rank0
    slot1 = r1.astype(F32) * C + rank1
    lane_s = lax.broadcasted_iota(jnp.int32, (R, S * C), 1).astype(F32)

    def picker(slot):
        return jnp.where(lane_s == slot, 1.0, 0.0)

    qi = lax.broadcasted_iota(jnp.int32, (R, R), 0)
    kj = lax.broadcasted_iota(jnp.int32, (R, R), 1)
    dist_own = (qi - kj).astype(F32)
    dist_old = (qi - kj + WINDOW).astype(F32)
    nt = (((1,), (1,)), ((), ()))

    ok_own = qi >= kj
    ok_old = (kj >= qi) & (kj + me * R >= WINDOW)

    def head(h):
        return slice(h * HEAD_DIM, (h + 1) * HEAD_DIM), slice(
            (h // G) * HEAD_DIM, (h // G + 1) * HEAD_DIM
        )

    def scores(h, keys, dist, ok):
        raw = lax.dot_general(q_ref[:, head(h)[0]], keys, nt, preferred_element_type=F32)
        return jnp.where(ok, raw * HEAD_DIM**-0.5 - slope_ref[t * H + h] * dist, -jnp.inf)

    own = [scores(h, k_ref[:, head(h)[1]], dist_own, ok_own) for h in range(H)]
    own_peak = [jnp.max(x, axis=1, keepdims=True) for x in own]

    @pl.when(me > 0)
    def _():
        for copy in halo_copies:
            copy.wait_recv()

    @pl.when(me == 0)
    def _():
        halo[...] = jnp.zeros_like(halo)

    for h in range(H):
        hc, kc = head(h)
        s_own = own[h]
        s_old = scores(h, halo[0, :, kc], dist_old, ok_old)
        peak = jnp.maximum(own_peak[h], jnp.max(s_old, axis=1, keepdims=True))
        e_own = jnp.exp(s_own - peak)
        e_old = jnp.exp(s_old - peak)
        total = jnp.sum(e_own, axis=1, keepdims=True) + jnp.sum(e_old, axis=1, keepdims=True)
        inv = 1.0 / total
        mix = jnp.dot((e_own * inv).astype(BF16), v_ref[:, kc], preferred_element_type=F32)
        mix += jnp.dot((e_old * inv).astype(BF16), halo[1, :, kc], preferred_element_type=F32)
        keep = 1.0 / (1.0 + jnp.exp(sink_ref[h] - peak - jnp.log(total)))
        att[:, hc] = (mix * keep).astype(BF16)

    loads[0].wait()

    def project(tt):
        pp[:, cols(tt)] = jnp.dot(att[...], wo[:, cols(tt)], preferred_element_type=F32).astype(
            BF16
        )

    def c1(yy):
        return remote(
            pp.at[:, cols(tp_of(yy, oc))], rc1.at[yy], c1_s.at[yy], c1_r.at[yy], tp=tp_of(y, oc)
        )

    def y1_send(yy):
        return remote(sb1.at[yy], ry1.at[y], y1_s.at[yy], y1_r.at[y], tp=tp_of(yy, c))

    def y1_recv(yy):
        return remote(sb1.at[yy], ry1.at[yy], y1_s.at[yy], y1_r.at[yy], tp=tp_of(yy, c))

    for d in list(range(1, Y)) + [0]:
        project(tp_of(yo(d), oc))
        c1(yo(d)).start()
    for d in list(range(1, Y)) + [0]:
        project(tp_of(yo(d), c))
    for d in range(1, Y):
        c1(yo(d)).wait_recv()
        sb1[yo(d)] = (pp[:, cols(tp_of(yo(d), c))].astype(F32) + rc1[yo(d)].astype(F32)).astype(
            BF16
        )
        y1_send(yo(d)).start()
    c1(y).wait_recv()
    head_sum = pp[:, cols(t)].astype(F32) + rc1[y].astype(F32)
    for d in range(1, Y):
        y1_recv(yo(d)).wait_recv()
        head_sum = head_sum + ry1[yo(d)].astype(F32)
    mixed[...] = (res_ref[:, cols(t)].astype(F32) + head_sum).astype(BF16)

    both = (picker(slot0) + picker(slot1)).T.astype(BF16)
    picked[...] = jnp.dot(both, mixed[...], preferred_element_type=F32).astype(BF16)

    loc = me // 2
    near = me % 2
    far = 1 - near

    def source(par, p):
        return 2 * p + par

    def place(par, d):
        return source(par, (loc + half - d) % half)

    def spot(s):
        return rows((s % 2) * half + s // 2)

    def a_send(e):
        return remote(
            picked.at[rows(e)], x_all.at[spot(me), cols(t)], a_s.at[e], a_r.at[me], sp=e
        )

    def a_recv(s):
        return remote(picked.at[rows(s)], x_all.at[spot(s), cols(t)], a_s.at[s], a_r.at[s], sp=s)

    def fy_send(s, yy):
        ref = x_all.at[spot(s), cols(t)]
        return remote(ref, ref, fy_s.at[s, yy], fy_r.at[s, y], tp=tp_of(yy, c))

    def fy_recv(s, yy):
        ref = x_all.at[spot(s), cols(tp_of(yy, c))]
        return remote(ref, ref, fy_s.at[s, yy], fy_r.at[s, yy], tp=tp_of(yy, c))

    def fc_send(s, yy):
        ref = x_all.at[spot(s), cols(tp_of(yy, c))]
        return remote(ref, ref, fc_s.at[s, yy], fc_r.at[s, yy], tp=tp_of(y, oc))

    def fc_recv(s, yy):
        ref = x_all.at[spot(s), cols(tp_of(yy, oc))]
        return remote(ref, ref, fc_s.at[s, yy], fc_r.at[s, yy], tp=tp_of(y, oc))

    @pl.loop(1, half)
    def _(d):
        a_send(source(near, (loc + d) % half)).start()

    @pl.loop(0, half)
    def _(d):
        a_send(source(far, (loc + d) % half)).start()

    x_all[spot(me), cols(t)] = picked[rows(me)]

    def forward(s):
        for d in range(1, Y):
            fy_send(s, yo(d)).start()
        fc_send(s, y).start()

    def relay(s):
        for i in range(1, Y):
            fy_recv(s, yo(i)).wait_recv()
            fc_send(s, yo(i)).start()

    def arrive(s):
        a_recv(s).wait_recv()
        forward(s)

    def norm_group(base):
        @pl.loop(0, half)
        def _(d):
            s = place(base, d)
            for i in range(Y):
                fc_recv(s, yo(i)).wait_recv()
            x = x_all[spot(s)].astype(F32)
            scale = lax.rsqrt(jnp.mean(x * x, axis=1, keepdims=True) + 1e-06)
            xn[spot(s)] = (x * scale * gain_ref[...]).astype(BF16)

    TN = min(256, FL)

    def hidden_group(base):
        at = pl.ds(pl.multiple_of(base * GM, GM), GM)

        @pl.loop(0, FL // TN)
        def _(n):
            nn = pl.ds(pl.multiple_of(n * TN, TN), TN)
            gate = jnp.dot(xn[at], wg[:, nn], preferred_element_type=F32)
            up = jnp.dot(xn[at], wu[:, nn], preferred_element_type=F32)
            act[:, nn] = (gate / (1.0 + jnp.exp(-gate)) * up).astype(BF16)

    def c2(g, yy):
        return remote(
            yp.at[g, :, cols(tp_of(yy, oc))],
            rc2.at[g, yy],
            c2_s.at[g, yy],
            c2_r.at[g, yy],
            tp=tp_of(y, oc),
        )

    def down_block(g, tt):
        yp[g, :, cols(tt)] = jnp.dot(act[...], wd[:, cols(tt)], preferred_element_type=F32).astype(
            BF16
        )

    def down_group(g):
        @pl.loop(0, Y)
        def _(d):
            yy = yo(d + 1)
            down_block(g, tp_of(yy, oc))
            c2(g, yy).start()

        @pl.loop(0, Y)
        def _(d):
            down_block(g, tp_of(yo(d + 1), c))

    def y2_send(g, p, yy):
        return remote(
            sb2.at[g, yy, rows(p)],
            ry2.at[g, y, rows(p)],
            y2_s.at[g, p, yy],
            y2_r.at[g, p, y],
            tp=tp_of(yy, c),
        )

    def y2_recv(g, p, yy):
        return remote(
            sb2.at[g, yy, rows(p)],
            ry2.at[g, yy, rows(p)],
            y2_s.at[g, p, yy],
            y2_r.at[g, p, yy],
            tp=tp_of(yy, c),
        )

    def b_send(s):
        return remote(rb.at[rows(s)], ret.at[rows(me)], b_s.at[s], b_r.at[me], sp=s)

    def b_recv(s):
        return remote(rb.at[rows(s)], ret.at[rows(s)], b_s.at[s], b_r.at[s], sp=s)

    def pair_sum(g):
        for d in list(range(1, Y)) + [0]:
            yy = yo(d)
            c2(g, yy).wait_recv()

            @pl.loop(0, half)
            def _(i):
                p = (loc + half - i) % half
                sb2[g, yy, rows(p)] = (
                    yp[g, rows(p), cols(tp_of(yy, c))].astype(F32) + rc2[g, yy, rows(p)].astype(F32)
                ).astype(BF16)
                if d:
                    y2_send(g, p, yy).start()

    def send_back(g, base):
        @pl.loop(0, half)
        def _(i):
            p = (loc + half - i) % half
            s = source(base, p)
            total = sb2[g, y, rows(p)].astype(F32)
            for d in range(1, Y):
                y2_recv(g, p, yo(d)).wait_recv()
                total = total + ry2[g, yo(d), rows(p)].astype(F32)
            rb[rows(s)] = total.astype(BF16)

            @pl.when(s != me)
            def _():
                b_send(s).start()

    forward(me)

    @pl.loop(1, half)
    def _(d):
        arrive(place(near, d))

    @pl.loop(0, half)
    def _(d):
        relay(place(near, d))
        arrive(place(far, d))

    norm_group(near)
    loads[1].wait()
    loads[2].wait()
    hidden_group(near)

    loads[3].wait()
    down_group(0)

    @pl.loop(0, half)
    def _(d):
        relay(place(far, d))

    pair_sum(0)
    norm_group(far)
    hidden_group(far)
    send_back(0, near)
    down_group(1)
    pair_sum(1)
    send_back(1, far)

    ret[rows(me)] = rb[rows(me)]

    @pl.loop(1, S)
    def _(d):
        b_recv((me + d) % S).wait_recv()

    mix0 = jnp.dot(picker(slot0).astype(BF16), ret[...], preferred_element_type=F32)
    mix1 = jnp.dot(picker(slot1).astype(BF16), ret[...], preferred_element_type=F32)
    o_all[:, cols(t)] = (
        mixed[...].astype(F32) + (column(rw_ref[0:1, :]) * mix0 + column(rw_ref[1:2, :]) * mix1)
    ).astype(BF16)

    def gy_send(yy):
        ref = o_all.at[:, cols(t)]
        return remote(ref, ref, gy_s.at[yy], gy_r.at[y], tp=tp_of(yy, c))

    def gy_recv(yy):
        ref = o_all.at[:, cols(tp_of(yy, c))]
        return remote(ref, ref, gy_s.at[yy], gy_r.at[yy], tp=tp_of(yy, c))

    def gc_send(yy):
        ref = o_all.at[:, cols(tp_of(yy, c))]
        return remote(ref, ref, gc_s.at[yy], gc_r.at[yy], tp=tp_of(y, oc))

    def gc_recv(yy):
        ref = o_all.at[:, cols(tp_of(yy, oc))]
        return remote(ref, ref, gc_s.at[yy], gc_r.at[yy], tp=tp_of(y, oc))

    for d in range(1, Y):
        gy_send(yo(d)).start()
    gc_send(y).start()
    for d in range(1, Y):
        gy_recv(yo(d)).wait_recv()
        gc_send(yo(d)).start()
    for d in range(Y):
        gc_recv(yo(d)).wait_recv()
    out_ref[...] = o_all[...]

    @pl.when(me < S - 1)
    def _():
        for copy in halo_copies:
            copy.wait_send()

    for d in range(Y):
        c1(yo(d)).wait_send()
        gc_send(yo(d)).wait_send()
        for g in range(2):
            c2(g, yo(d)).wait_send()
    for d in range(1, Y):
        y1_send(yo(d)).wait_send()
        gy_send(yo(d)).wait_send()

    @pl.loop(1, S)
    def _(d):
        a_send((me + d) % S).wait_send()
        b_send((me + d) % S).wait_send()

    @pl.loop(0, S)
    def _(s):
        for d in range(Y):
            fc_send(s, yo(d)).wait_send()
        for d in range(1, Y):
            fy_send(s, yo(d)).wait_send()

    @pl.loop(0, half)
    def _(p):
        for d in range(1, Y):
            for g in range(2):
                y2_send(g, p, yo(d)).wait_send()


def per_device(
    S,
    T,
    queries,
    key_rows,
    value_rows,
    sink_logits,
    out_weight,
    residual,
    norm_gain,
    routes,
    route_weights,
    gate_weight,
    up_weight,
    down_weight,
):
    R, D = residual.shape
    HW = queries.shape[1]
    heads = HW // HEAD_DIM * T
    Y = T // CORES
    W = D // T
    C = 2 * R * TOP // S
    half = S // 2
    GM = half * C
    FL = gate_weight.shape[2]
    slopes = jnp.asarray(np.exp2(-8.0 * np.arange(1, heads + 1) / heads).astype(np.float32))
    vmem = pl.BlockSpec(memory_space=pltpu.VMEM)
    smem = pl.BlockSpec(memory_space=pltpu.SMEM)
    hbm = pl.BlockSpec(memory_space=pl.ANY)
    dma = pltpu.SemaphoreType.DMA
    v = pltpu.VMEM
    return pl.pallas_call(
        functools.partial(kernel, S, T),
        out_shape=jax.ShapeDtypeStruct((R, D), BF16),
        in_specs=[smem, smem] + [vmem] * 7 + [hbm] * 4,
        out_specs=vmem,
        scratch_shapes=[
            v(out_weight.shape, BF16),
            v(gate_weight.shape[1:], BF16),
            v(up_weight.shape[1:], BF16),
            v(down_weight.shape[1:], BF16),
            v((2,) + key_rows.shape, BF16),
            v((R, HW), BF16),
            v((R, D), BF16),
            v((Y, R, W), BF16),
            v((Y, R, W), BF16),
            v((Y, R, W), BF16),
            v((R, W), BF16),
            v((S * C, W), BF16),
            v((S * C, D), BF16),
            v((S * C, D), BF16),
            v((GM, FL), BF16),
            v((2, GM, D), BF16),
            v((2, Y, GM, W), BF16),
            v((2, Y, GM, W), BF16),
            v((2, Y, GM, W), BF16),
            v((S * C, W), BF16),
            v((S * C, W), BF16),
            v((R, D), BF16),
            dma((4,)),
            dma((2,)),
            dma((2,)),
            dma((Y,)),
            dma((Y,)),
            dma((Y,)),
            dma((Y,)),
            dma((S,)),
            dma((S,)),
            dma((S, Y)),
            dma((S, Y)),
            dma((S, Y)),
            dma((S, Y)),
            dma((2, Y)),
            dma((2, Y)),
            dma((2, half, Y)),
            dma((2, half, Y)),
            dma((S,)),
            dma((S,)),
            dma((Y,)),
            dma((Y,)),
            dma((Y,)),
            dma((Y,)),
        ],
        compiler_params=pltpu.CompilerParams(
            collective_id=0, has_side_effects=True, vmem_limit_bytes=60 * 1024 * 1024
        ),
        name="layer",
    )(
        slopes,
        sink_logits,
        queries,
        key_rows,
        value_rows,
        residual,
        norm_gain.reshape(1, D),
        routes.T,
        route_weights.T,
        out_weight,
        gate_weight,
        up_weight,
        down_weight,
    )


def solution(mesh):
    placed = (
        P("sp", "tp"),
        P("sp", "tp"),
        P("sp", "tp"),
        P("tp"),
        P("tp", None),
        P("sp", None),
        P(),
        P("sp", None),
        P("sp", None),
        P("sp", None, "tp"),
        P("sp", None, "tp"),
        P("sp", "tp", None),
    )
    return jax.shard_map(
        functools.partial(per_device, mesh.shape["sp"], mesh.shape["tp"]),
        mesh=mesh,
        in_specs=placed,
        out_specs=P("sp", None),
        check_vma=False,
    )
```
